32 devices in a mesh: sp: 8 (over z, x), tp: 4 (over y, core).
Axes of the slice: x: 2, y: 2, z: 4, core: 2. Of those that a mesh axis runs over, the one named last changes fastest.
Arguments:
- query_wide: bfloat16 [6144, 8, 256], P('sp', 'tp'), may hold values from -6 to 6
- key_wide: bfloat16 [6144, 8, 256], P('sp', 'tp'), may hold values from -6 to 6
- value_wide: bfloat16 [6144, 8, 256], P('sp', 'tp'), may hold values from -6 to 6
- query_narrow: bfloat16 [6144, 8, 128], P('sp', 'tp'), may hold values from -6 to 6
- key_narrow: bfloat16 [6144, 8, 128], P('sp', 'tp'), may hold values from -6 to 6
- value_narrow: bfloat16 [6144, 8, 128], P('sp', 'tp'), may hold values from -6 to 6
- mix_lambda: float32 [2, 8], P(None, 'tp'), may hold values from 0.3 to 0.8
- residual_in: bfloat16 [6144, 2048], P(('sp', 'tp')), may hold values from -6 to 6
- out_wide: bfloat16 [2048, 2048], P('tp'), may hold values from -0.109375 to 0.109375
- out_narrow: bfloat16 [1024, 2048], P('tp'), may hold values from -0.109375 to 0.109375
- ffn_gain: float32 [2048], replicated, may hold values from 0.1 to 1.9
- expert_ids: int32 [6144, 2], P(('sp', 'tp')), may hold values from 0 to 31, as said below
- expert_weights: float32 [6144, 2], P(('sp', 'tp')), may hold values from 0.1 to 1
- gate_weight: bfloat16 [32, 2048, 1024], P(('sp', 'tp')), may hold values from -0.125 to 0.125
- up_weight: bfloat16 [32, 2048, 1024], P(('sp', 'tp')), may hold values from -0.125 to 0.125
- down_weight: bfloat16 [32, 1024, 2048], P(('sp', 'tp')), may hold values from -0.1875 to 0.1875
Outputs:
- layer_out: bfloat16 [6144, 2048], P(('sp', 'tp'))
The draws below stay inside these ranges and needn't reach their ends.
Inputs may be any that keep to these rules, and one draw needn't show every extreme that they name: `expert_ids`: A row's two experts differ and lie in the same group of 4 consecutive experts (8 groups). In each aligned block of 192 rows (the rows of one device) no expert is named by more than 24 rows, and in every block some expert is named by exactly 24 rows.
All inputs are finite; a program needn't handle non-finite values.
Results may differ from the reference program's by a relative error of at most 0.015.
Values may be sent and summed in bfloat16 or wider, within the bound.
A program may use at most 192 MiB of HBM per device.

```python
import math
import jax
import jax.numpy as jnp
from jax import lax

D = 2048
HEADS = 8
DA = 128
DB = 64
VA = 256
VB = 128
FF = 1024
GROUP_SIZE = 4
TOKENS = 6144
TOK_LOC = 192
EXPERTS = 32
CAP = 24


def query_draw(key, salt, head_size):
    values_drawn = jnp.clip(jax.random.normal(jax.random.fold_in(key, salt + 100), (TOKENS, HEADS, 2 * head_size), jnp.float32) * 1.3, -6.0, 6.0)
    return values_drawn.astype(jnp.bfloat16)


def key_draw(key, salt, head_size):
    values_drawn = jnp.clip(jax.random.normal(jax.random.fold_in(key, salt + 200), (TOKENS, HEADS, 2 * head_size), jnp.float32) * 1.3, -6.0, 6.0)
    return values_drawn.astype(jnp.bfloat16)


def draw_query_wide(key, part):
    return query_draw(key, 5, DA)


def draw_key_wide(key, part):
    return key_draw(key, 5, DA)


def draw_query_narrow(key, part):
    return query_draw(key, 9, DB)


def draw_key_narrow(key, part):
    return key_draw(key, 9, DB)


def draw_expert_ids(key, part):
    positions = EXPERTS * CAP // 2
    blocks = TOKENS // TOK_LOC
    forced = jax.random.randint(jax.random.fold_in(key, 31), (), 0, EXPERTS)
    pair_first = jnp.array([[0, 2], [0, 1], [0, 1]], jnp.int32)
    pair_second = jnp.array([[1, 3], [2, 3], [3, 2]], jnp.int32)

    def one_block(block_key):
        key_kind, key_score, key_order, key_flip = jax.random.split(block_key, 4)
        position = jnp.arange(positions, dtype=jnp.int32)
        group_index = position // (2 * CAP)
        level_index = position % (2 * CAP) // 2
        which_pair = position % 2
        pair_kind = jax.random.randint(key_kind, (EXPERTS // GROUP_SIZE, CAP), 0, 3)
        kinds = pair_kind[group_index, level_index]
        first_expert = pair_first[kinds, which_pair] + group_index * GROUP_SIZE
        second_expert = pair_second[kinds, which_pair] + group_index * GROUP_SIZE
        hit = ((first_expert == forced) | (second_expert == forced)).astype(jnp.int32)
        priority = jax.random.randint(key_score, (positions,), 0, 2 ** 20) * 1024 + position + hit * 2 ** 30
        _, chosen = lax.top_k(priority, TOK_LOC)
        shuffle = jax.random.permutation(key_order, TOK_LOC)
        picked = chosen[shuffle]
        flipped = jax.random.randint(key_flip, (TOK_LOC,), 0, 2)
        left_expert = first_expert[picked]
        right_expert = second_expert[picked]
        low_expert = jnp.where(flipped == 1, right_expert, left_expert)
        high_expert = jnp.where(flipped == 1, left_expert, right_expert)
        return jnp.stack([low_expert, high_expert], axis=-1)
    block_keys = jax.random.split(jax.random.fold_in(key, 32), blocks)
    return jax.vmap(one_block)(block_keys).reshape(TOKENS, 2).astype(jnp.int32)


def steps_of(stream_key, dims, cuts, smallest, top_value):
    gain, own = 1.0, jax.random.fold_in(stream_key, 6)
    for dim, shards_of in cuts:
        steps = jnp.exp(jax.random.uniform(jax.random.fold_in(own, dim), (shards_of,), jnp.float32, smallest / len(cuts), top_value / len(cuts)))
        gain = gain * jnp.repeat(steps, dims[dim] // shards_of).reshape([-1 if axis == dim else 1 for axis in range(len(dims))])
    return gain


def centred(stream_key, dims, spread, reach, pieces=(), kind=jnp.bfloat16):
    values = spread * jax.random.normal(stream_key, dims, jnp.float32)
    if pieces:
        values = values * steps_of(stream_key, dims, pieces, -0.22, 0.18)
    return jnp.clip(values, -reach, reach).astype(kind)


def setup_inputs(seed: int = 0) -> dict:
    streams_of = jax.random.split(jax.random.key(seed), 17)
    return {
        "query_wide": draw_query_wide(jax.random.fold_in(streams_of[16], 71), 0),
        "key_wide": draw_key_wide(jax.random.fold_in(streams_of[16], 71), 0),
        "value_wide": centred(streams_of[2], (TOKENS, HEADS, VA), 1.0, 6.0, ((0, 8), (1, 4))),
        "query_narrow": draw_query_narrow(jax.random.fold_in(streams_of[16], 71), 0),
        "key_narrow": draw_key_narrow(jax.random.fold_in(streams_of[16], 71), 0),
        "value_narrow": centred(streams_of[5], (TOKENS, HEADS, VB), 1.0, 6.0, ((0, 8), (1, 4))),
        "mix_lambda": jnp.clip(0.3 + 0.5 * jax.random.uniform(streams_of[6], (2, HEADS), jnp.float32) ** steps_of(streams_of[6], (2, HEADS), ((1, 4),), -0.2, 0.2), 0.3, 0.8),
        "residual_in": centred(streams_of[7], (TOKENS, D), 1.0, 6.0, ((0, 32),)),
        "out_wide": centred(streams_of[8], (HEADS * VA, D), (HEADS * VA + HEADS * VB) ** -0.5, 0.109375, ((0, 4),)),
        "out_narrow": centred(streams_of[9], (HEADS * VB, D), (HEADS * VA + HEADS * VB) ** -0.5, 0.109375, ((0, 4),)),
        "ffn_gain": jnp.clip(1.0 + 0.18 * jax.random.normal(streams_of[10], (D,), jnp.float32), 0.1, 1.9),
        "expert_ids": draw_expert_ids(jax.random.fold_in(streams_of[16], 71), 0),
        "expert_weights": jnp.clip(0.1 + 0.9 * jax.random.uniform(streams_of[12], (TOKENS, 2), jnp.float32) ** steps_of(streams_of[12], (TOKENS, 2), ((0, 32),), -0.2, 0.2), 0.1, 1.0),
        "gate_weight": centred(streams_of[13], (EXPERTS, D, FF), D ** -0.5, 0.125, ((0, 32),)),
        "up_weight": centred(streams_of[14], (EXPERTS, D, FF), D ** -0.5, 0.125, ((0, 32),)),
        "down_weight": centred(streams_of[15], (EXPERTS, FF, D), FF ** -0.5, 0.1875, ((0, 32),)),
    }


def head_group(query, keys, values, lam_row, head_size):
    score_scale = head_size ** (-0.5)
    query_block = math.gcd(TOKENS, 512)
    query_f = query.astype(jnp.float32)
    keys_f = keys.astype(jnp.float32)
    values_f = values.astype(jnp.float32)
    key_pos = jnp.arange(TOKENS, dtype=jnp.int32)

    def block_read(number):
        query_rows = lax.dynamic_slice_in_dim(query_f, number * query_block, query_block, 0)
        query_pos = number * query_block + jnp.arange(query_block, dtype=jnp.int32)
        causal = key_pos[None, :] <= query_pos[:, None]
        reads = []
        for which_map in range(2):
            lower_edge = which_map * head_size
            scores = jnp.einsum('qhd,khd->hqk', query_rows[..., lower_edge:lower_edge + head_size], keys_f[..., lower_edge:lower_edge + head_size]) * score_scale
            scores = jnp.where(causal[None], scores, -jnp.inf)
            new_peak = lax.optimization_barrier(jnp.max(scores, axis=-1, keepdims=True))
            expo = jnp.exp(scores - new_peak)
            totals = lax.optimization_barrier(jnp.sum(expo, axis=-1))
            rounded = lax.optimization_barrier(expo.astype(jnp.bfloat16)).astype(jnp.float32)
            reads.append(jnp.einsum('hqk,khv->hqv', rounded, values_f) / totals[..., None])
        mixed_read = reads[0] - lam_row[:, None, None] * reads[1]
        normed = mixed_read * lax.rsqrt(lax.optimization_barrier(jnp.mean(mixed_read * mixed_read, axis=-1, keepdims=True)) + 1e-06)
        return jnp.transpose(normed.astype(jnp.bfloat16), (1, 0, 2))
    outputs = lax.map(block_read, jnp.arange(TOKENS // query_block, dtype=jnp.int32))
    return outputs.reshape(TOKENS, -1)

def reference(query_wide, key_wide, value_wide, query_narrow, key_narrow, value_narrow, mix_lambda, residual_in, out_wide, out_narrow, ffn_gain, expert_ids, expert_weights, gate_weight, up_weight, down_weight):
    heads_wide = head_group(query_wide, key_wide, value_wide, mix_lambda[0], DA)
    heads_narrow = head_group(query_narrow, key_narrow, value_narrow, mix_lambda[1], DB)
    projected = jnp.dot(heads_wide, out_wide, preferred_element_type=jnp.float32) + jnp.dot(heads_narrow, out_narrow, preferred_element_type=jnp.float32)
    stream = (projected + residual_in.astype(jnp.float32)).astype(jnp.bfloat16)
    stream_f = stream.astype(jnp.float32)
    normed = (stream_f * lax.rsqrt(lax.optimization_barrier(jnp.mean(stream_f * stream_f, axis=-1, keepdims=True)) + 1e-06) * ffn_gain).astype(jnp.bfloat16)
    flat_expert = expert_ids.reshape(-1)
    flat_token = jnp.repeat(jnp.arange(TOKENS, dtype=jnp.int32), 2)
    flat_weight = expert_weights.reshape(-1)
    slots = EXPERTS * CAP

    def one_expert(running, expert):
        chosen = flat_expert == expert
        count = jnp.sum(chosen.astype(jnp.int32))
        position = jnp.nonzero(chosen, size=slots, fill_value=0)[0].astype(jnp.int32)
        token_rows = flat_token[position]
        rows = normed[token_rows]
        gate_part = jnp.dot(rows, gate_weight[expert], preferred_element_type=jnp.float32)
        up_part = jnp.dot(rows, up_weight[expert], preferred_element_type=jnp.float32)
        hidden = (jax.nn.silu(gate_part) * up_part).astype(jnp.bfloat16)
        result = jnp.dot(hidden, down_weight[expert], preferred_element_type=jnp.float32)
        result = lax.optimization_barrier(result.astype(jnp.bfloat16)).astype(jnp.float32)
        share = jnp.where(jnp.arange(slots, dtype=jnp.int32) < count, flat_weight[position], 0.0)
        return (running.at[token_rows].add(share[:, None] * result), None)
    summed, _ = lax.scan(one_expert, jnp.zeros((TOKENS, D), jnp.float32), jnp.arange(EXPERTS, dtype=jnp.int32))
    return (stream_f + summed).astype(jnp.bfloat16)
```

```python
import functools
import math

import jax
import jax.numpy as jnp
from jax import lax
from jax.experimental import pallas as pl
from jax.experimental.pallas import tpu as pltpu
from jax.sharding import PartitionSpec as P

NEG_FILL = -1e30


def attend_kernel(flags, lam, *refs, count, diag, final, head_size, packed):
    q_ref = refs[0]
    blocks = [(refs[1 + 2 * b], refs[2 + 2 * b]) for b in range(count)]
    refs = refs[1 + 2 * count :]
    if not diag:
        acc_in, stat_in = refs[:2]
        refs = refs[2:]
    if final:
        out_ref, acc, peak, total = refs
    else:
        acc_out, stat_out, acc, peak, total = refs
    scale = head_size ** (-0.5) * math.log2(math.e)
    rows = q_ref.shape[0]
    head = pl.program_id(0)
    first_row = pl.program_id(1) * rows

    def lanes(column):
        return jnp.broadcast_to(column, (rows, 128))

    if not diag:
        acc[...] = acc_in[...]
        for m in range(2):
            peak[m] = lanes(stat_in[0, :, 2 * m : 2 * m + 1])
            total[m] = lanes(stat_in[0, :, 2 * m + 1 : 2 * m + 2])

    def update(k_ref, v_ref):
        values = v_ref[...]
        for m in range(2):
            if packed:
                side = lax.broadcasted_iota(jnp.int32, q_ref.shape, 1) // head_size
                query = jnp.where(side == m, q_ref[...], jnp.zeros_like(q_ref))
                keys = k_ref[...]
            else:
                query = q_ref[:, m * head_size : (m + 1) * head_size]
                keys = k_ref[:, m * head_size : (m + 1) * head_size]
            scores = (
                lax.dot_general(
                    query, keys, (((1,), (1,)), ((), ())), preferred_element_type=jnp.float32
                )
                * scale
            )
            if diag:
                row = first_row + lax.broadcasted_iota(jnp.int32, scores.shape, 0)
                col = lax.broadcasted_iota(jnp.int32, scores.shape, 1)
                scores = jnp.where(col <= row, scores, NEG_FILL)
            new_peak = jnp.max(scores, axis=1, keepdims=True)
            if not diag:
                old_peak = peak[m][:, :1]
                new_peak = jnp.maximum(old_peak, new_peak)
                factor = jnp.exp2(old_peak - new_peak)
            weights = jnp.exp2(scores - new_peak)
            new_total = jnp.sum(weights, axis=1, keepdims=True)
            read = jnp.dot(
                weights.astype(jnp.bfloat16), values, preferred_element_type=jnp.float32
            )
            if not diag:
                new_total = new_total + factor * total[m][:, :1]
                read = read + factor * acc[m]
            acc[m] = read
            peak[m] = lanes(new_peak)
            total[m] = lanes(new_total)

    for b in range(count):
        if diag:
            update(*blocks[b])
        else:
            pl.when(flags[b] == 1)(functools.partial(update, *blocks[b]))

    if final:
        mixed = acc[0] / total[0][:, :1] - lam[head] * (acc[1] / total[1][:, :1])
        out_ref[...] = (
            mixed * lax.rsqrt(jnp.mean(mixed * mixed, axis=1, keepdims=True) + 1e-06)
        ).astype(out_ref.dtype)
    else:
        acc_out[...] = acc[...]
        lane = lax.broadcasted_iota(jnp.int32, (rows, 128), 1)
        stat_out[0] = jnp.where(
            lane == 0,
            peak[0],
            jnp.where(lane == 1, total[0], jnp.where(lane == 2, peak[1], total[1])),
        )


def attend(query, pieces, flags, state, lam, head_size, value_size, key_col, value_col, final):
    diag = state is None
    tok_count, width = query.shape
    heads = width // (2 * head_size)
    block = math.gcd(tok_count, 256)
    packed = head_size % 128 != 0
    kb, vb = key_col // (2 * head_size), value_col // value_size
    q_spec = pl.BlockSpec((block, 2 * head_size), lambda h, i, *_: (i, h))
    acc_spec = pl.BlockSpec((2, block, value_size), lambda h, i, *_: (0, i, h))
    stat_spec = pl.BlockSpec((1, block, 128), lambda h, i, *_: (h, i, 0))
    in_specs, operands = [q_spec], [query]
    keys_seen = 0
    for piece, start, rows in pieces:
        keys_seen += rows
        at = start // rows
        in_specs += [
            pl.BlockSpec((rows, 2 * head_size), lambda h, i, *_, at=at: (at, kb + h)),
            pl.BlockSpec((rows, value_size), lambda h, i, *_, at=at: (at, vb + h)),
        ]
        operands += [piece, piece]
    aliases = {}
    if not diag:
        in_specs += [acc_spec, stat_spec]
        operands += list(state)
        if not final:
            aliases = {2 + len(operands) - 2: 0, 2 + len(operands) - 1: 1}
    if final:
        out_specs = pl.BlockSpec((block, value_size), lambda h, i, *_: (i, h))
        out_shape = jax.ShapeDtypeStruct((tok_count, heads * value_size), jnp.bfloat16)
    else:
        out_specs = (acc_spec, stat_spec)
        out_shape = (
            jax.ShapeDtypeStruct((2, tok_count, heads * value_size), jnp.float32),
            jax.ShapeDtypeStruct((heads, tok_count, 128), jnp.float32),
        )
    pairs = heads * tok_count * keys_seen * 2
    return pl.pallas_call(
        functools.partial(
            attend_kernel,
            count=len(pieces),
            diag=diag,
            final=final,
            head_size=head_size,
            packed=packed,
        ),
        grid_spec=pltpu.PrefetchScalarGridSpec(
            num_scalar_prefetch=2,
            grid=(heads, tok_count // block),
            in_specs=in_specs,
            out_specs=out_specs,
            scratch_shapes=[
                pltpu.VMEM((2, block, value_size), jnp.float32),
                pltpu.VMEM((2, block, 128), jnp.float32),
                pltpu.VMEM((2, block, 128), jnp.float32),
            ],
        ),
        out_shape=out_shape,
        input_output_aliases=aliases,
        compiler_params=pltpu.CompilerParams(vmem_limit_bytes=40 * 1024 * 1024),
        cost_estimate=pl.CostEstimate(
            flops=pairs * 1024,
            bytes_accessed=keys_seen * heads * (2 * head_size + value_size) * 2
            + tok_count * heads * value_size * 16,
            transcendentals=pairs,
        ),
    )(flags, lam, *operands)


def ring_order(count):
    return list(range(0, count, 2)) + list(range(1, count, 2))[::-1]


def shards(
    query_wide,
    key_wide,
    value_wide,
    query_narrow,
    key_narrow,
    value_narrow,
    mix_lambda,
    residual_in,
    out_wide,
    out_narrow,
    ffn_gain,
    expert_ids,
    expert_weights,
    gate_weight,
    up_weight,
    down_weight,
):
    tok_count, local_heads, _ = query_wide.shape
    size_wide = query_wide.shape[2] // 2
    size_narrow = query_narrow.shape[2] // 2

    value_wide_size, value_narrow_size = value_wide.shape[2], value_narrow.shape[2]
    flat = lambda member: member.reshape(tok_count, -1)
    own = jnp.concatenate(
        [flat(key_wide), flat(value_wide), flat(key_narrow), flat(value_narrow)], axis=1
    )
    wide_q, narrow_q = flat(query_wide), flat(query_narrow)
    wide_v_col = local_heads * 2 * size_wide
    narrow_k_col = wide_v_col + local_heads * value_wide_size
    narrow_v_col = narrow_k_col + local_heads * 2 * size_narrow

    count = lax.axis_size("sp")
    order = ring_order(count)
    place = [order.index(device) for device in range(count)]
    me = lax.axis_index("sp")
    order_table = jnp.array(order, jnp.int32)
    my_place = jnp.array(place, jnp.int32)[me]
    forward = [(order[i], order[(i + 1) % count]) for i in range(count)]
    backward = [(b, a) for a, b in forward]

    def source_flag(shift):
        return (order_table[(my_place + shift) % count] < me).astype(jnp.int32)

    def both(pieces, flags, states, final=False):
        return (
            attend(
                wide_q, pieces, flags, states[0], mix_lambda[0], size_wide, value_wide_size,
                0, wide_v_col, final,
            ),
            attend(
                narrow_q, pieces, flags, states[1], mix_lambda[1], size_narrow, value_narrow_size,
                narrow_k_col, narrow_v_col, final,
            ),
        )

    half = tok_count // 2
    pieces = [(own, 0, tok_count)]
    flags = jnp.ones((2,), jnp.int32)
    states = (None, None)
    left = right = own
    for step in range(1, count // 2 + 1):
        if step < count // 2:
            left = lax.ppermute(left, "sp", forward)
            right = lax.ppermute(right, "sp", backward)
            coming = [(left, 0, tok_count), (right, 0, tok_count)]
        else:
            coming = [
                (lax.ppermute(left[:half], "sp", forward), 0, half),
                (lax.ppermute(right[half:], "sp", backward), 0, half),
            ]
        states = both(pieces, flags, states)
        arrived_now, states = lax.optimization_barrier(
            (tuple(piece for piece, _, _ in coming), states)
        )
        pieces = [(arrived_now[i], 0, coming[i][2]) for i in range(2)]
        left, right = arrived_now
        flags = jnp.stack([source_flag(-step), source_flag(step)])
    heads_wide, heads_narrow = both(pieces, flags, states, final=True)
    tp_size = lax.axis_size("tp")
    local_rows = tok_count // tp_size
    whole_wide, whole_narrow = (
        lax.all_gather(out_wide, "tp", axis=0, tiled=True),
        lax.all_gather(out_narrow, "tp", axis=0, tiled=True),
    )
    mine_wide, mine_narrow = (
        lax.all_to_all(heads_wide, "tp", split_axis=0, concat_axis=1, tiled=True),
        lax.all_to_all(heads_narrow, "tp", split_axis=0, concat_axis=1, tiled=True),
    )
    projected = jnp.dot(mine_wide, whole_wide, preferred_element_type=jnp.float32) + jnp.dot(
        mine_narrow, whole_narrow, preferred_element_type=jnp.float32
    )
    stream = (projected + residual_in.astype(jnp.float32)).astype(jnp.bfloat16)
    stream_f = stream.astype(jnp.float32)
    normed = (
        stream_f
        * lax.rsqrt(jnp.mean(stream_f * stream_f, axis=-1, keepdims=True) + 1e-06)
        * ffn_gain
    ).astype(jnp.bfloat16)
    experts_all = lax.axis_size("sp") * tp_size
    capacity = max(2, 4 * local_rows // experts_all)
    model_width = normed.shape[1]
    flat_expert = expert_ids.reshape(-1)
    expert_hot = (flat_expert[:, None] == jnp.arange(experts_all, dtype=jnp.int32)[None, :]).astype(
        jnp.int32
    )
    slot_rank = jnp.sum((jnp.cumsum(expert_hot, axis=0) - 1) * expert_hot, axis=1)
    flat_slot = flat_expert * capacity + slot_rank
    slot_ids = jnp.arange(experts_all * capacity, dtype=jnp.int32)
    placed = slot_ids[:, None] == flat_slot[None, :]
    dispatch = jnp.any(placed.reshape(experts_all * capacity, local_rows, 2), axis=2).astype(
        jnp.bfloat16
    )
    outgoing = jnp.dot(dispatch, normed, preferred_element_type=jnp.float32).astype(jnp.bfloat16)
    outgoing = outgoing.reshape(experts_all, capacity, model_width)
    arrived = lax.all_to_all(outgoing, ("sp", "tp"), split_axis=0, concat_axis=0, tiled=True)
    sources, items, width = arrived.shape
    flat_rows = arrived.reshape(sources * items, width)
    gate_part = jnp.dot(flat_rows, gate_weight[0], preferred_element_type=jnp.float32)
    up_part = jnp.dot(flat_rows, up_weight[0], preferred_element_type=jnp.float32)
    hidden = (jax.nn.silu(gate_part) * up_part).astype(jnp.bfloat16)
    result = jnp.dot(hidden, down_weight[0], preferred_element_type=jnp.float32).astype(
        jnp.bfloat16
    )
    returned = lax.all_to_all(
        result.reshape(sources, items, width), ("sp", "tp"), split_axis=0, concat_axis=0, tiled=True
    )
    slot_hot = (flat_slot[:, None] == slot_ids[None, :]).astype(
        jnp.float32
    ) * expert_weights.reshape(-1)[:, None]
    combine = jnp.sum(slot_hot.reshape(local_rows, 2, experts_all * capacity), axis=1)
    summed = jnp.dot(
        combine,
        returned.reshape(experts_all * capacity, model_width).astype(jnp.float32),
        precision=lax.Precision.HIGHEST,
    )
    return (stream_f + summed).astype(jnp.bfloat16)


def solution(mesh):
    return jax.shard_map(
        shards,
        mesh=mesh,
        in_specs=(
            P("sp", "tp", None),
            P("sp", "tp", None),
            P("sp", "tp", None),
            P("sp", "tp", None),
            P("sp", "tp", None),
            P("sp", "tp", None),
            P(None, "tp"),
            P(("sp", "tp"), None),
            P("tp", None),
            P("tp", None),
            P(),
            P(("sp", "tp"), None),
            P(("sp", "tp"), None),
            P(("sp", "tp"), None, None),
            P(("sp", "tp"), None, None),
            P(("sp", "tp"), None, None),
        ),
        out_specs=P(("sp", "tp"), None),
        check_vma=False,
    )
```
